32 devices in a mesh: grp: 2 (over x), st: 4 (over y, core), tp: 4 (over z).
Axes of the slice: x: 2, y: 2, z: 4, core: 2. Of those that a mesh axis runs over, the one named last changes fastest.
Arguments:
- tokens: bfloat16 [8192, 2048], P(('grp', 'st')), parts along dimension 0, may hold values from -6 to 6
- w_query: bfloat16 [2048, 512], P(None, 'tp'), may hold values from -0.125 to 0.125
- w_key: bfloat16 [2048, 512], P(None, 'tp'), may hold values from -0.125 to 0.125
- w_value: bfloat16 [2048, 1024], P(None, 'tp'), may hold values from -0.125 to 0.125
- w_decay: bfloat16 [2048, 512], P(None, 'tp'), may hold values from -0.125 to 0.125
- decay_rate: float32 [512], P('tp'), may hold values from 0.0002 to 0.04
- block_scale: float32 [64], P(('grp', 'st')), parts along dimension 0, may hold values from 0.5 to 2
- w_rquery: bfloat16 [2048, 1024], P(None, 'tp'), may hold values from -0.125 to 0.125
- w_gate: bfloat16 [2048, 1024], P(None, 'tp'), may hold values from -0.125 to 0.125
- w_rkey: bfloat16 [2048, 1024], P(None, 'tp'), may hold values from -0.125 to 0.125
- w_rvalue: bfloat16 [2048, 1024], P(None, 'tp'), may hold values from -3 to 3
- query_gain: float32 [128], replicated, may hold values from 0.1 to 1.9
- key_gain: float32 [128], replicated, may hold values from 0.1 to 1.9
- out_gain: float32 [1024], P('tp'), may hold values from 0.1 to 1.9
- store: bfloat16 [96, 128, 2048], P(('grp', 'st')), parts along dimension 0, may hold values from -6 to 6
- passage_ids: int32 [64, 4], P(('grp', 'st')), parts along dimension 0, may hold values from 0 to 47, as said below
Outputs:
- output: bfloat16 [8192, 1024], P(('grp', 'st'), 'tp'), parts along dimension 0
The draws below stay inside these ranges and needn't reach their ends.
There are 2 independent parts, one for each index of `grp`. The reference program is written for one: setup_inputs(seed, part) draws one part's arguments, and reference() takes and returns one part's arrays. A program takes and returns all parts, laid end to end along the dimension named above; an argument that names none is the same for every part. Nothing has to cross between parts.
Inputs may be any that keep to these rules, and one draw needn't show every extreme that they name: `passage_ids`: passage p is held by index p // 12 of st. The 32 reads of the blocks of one index of st name passages of exactly 4 indices of st, exactly 8 reads of each; among them are always the index before its own and the index half the axis away.
All inputs are finite; a program needn't handle non-finite values.
Results may differ from the reference program's by a relative error of at most 0.0044.
Values may be sent and summed in bfloat16 or wider, within the bound.
A program may use at most 128 MiB of HBM per device.

```python
import math
import jax
import jax.numpy as jnp
from jax import lax

D = 2048
HEADS = 8
DK = 64
DV = 128
LEN = 1024
BLK = 128
NPASS = 4
PLEN = 128
PASS_DEV = 12
TOKENS = 4096
BLOCKS = 8
REQS = 32
OWNERS = 4
MOST = 8
PASSAGES = 48
N_ST = 4


def draw_passage_ids(key, part):

    def one_index(index_key, device_index):
        key_pool, key_order, key_first, key_second = jax.random.split(index_key, 4)
        offset_pool = jax.random.permutation(key_pool, N_ST - 2).astype(jnp.int32)
        offset_pool = jnp.where(offset_pool < N_ST // 2, offset_pool, offset_pool + 1)
        forced = jnp.array([N_ST - 1, N_ST // 2], jnp.int32)
        offsets = jnp.concatenate([forced, offset_pool])[:OWNERS]
        request_order = jax.random.permutation(key_order, REQS).astype(jnp.int32)
        owner_index = (device_index + offsets[request_order // MOST]) % N_ST
        draw_first = jax.random.randint(key_first, (REQS,), 0, PASS_DEV, dtype=jnp.int32)
        draw_second = jax.random.randint(key_second, (REQS,), 0, PASS_DEV, dtype=jnp.int32)
        local_row = jnp.minimum(draw_first, draw_second)
        return (owner_index * PASS_DEV + local_row).reshape(BLOCKS, NPASS)
    index_keys = jax.random.split(key, N_ST)
    drawn = jax.vmap(one_index)(index_keys, jnp.arange(N_ST, dtype=jnp.int32))
    return drawn.reshape(N_ST * BLOCKS, NPASS).astype(jnp.int32)


def draw_decay_rate(key, part):
    key_kind, key_slow, key_fast = jax.random.split(key, 3)
    fast_cut = 8
    is_fast = jax.random.randint(key_kind, (HEADS,), 0, 16) < fast_cut
    slow_rate = jnp.exp(jax.random.uniform(key_slow, (HEADS, DK), jnp.float32, jnp.log(0.0002), jnp.log(0.0008)))
    fast_rate = jnp.exp(jax.random.uniform(key_fast, (HEADS, DK), jnp.float32, jnp.log(0.015), jnp.log(0.04)))
    return jnp.where(is_fast[:, None], fast_rate, slow_rate).reshape(HEADS * DK).astype(jnp.float32)


def level_of(stream_key, dims, cuts, smallest, largest):
    factor_of, own = 1.0, jax.random.fold_in(stream_key, 6)
    for position, blocks in cuts:
        steps = jnp.exp(jax.random.uniform(jax.random.fold_in(own, position), (blocks,), jnp.float32, smallest / len(cuts), largest / len(cuts)))
        factor_of = factor_of * jnp.repeat(steps, dims[position] // blocks).reshape([-1 if axis == position else 1 for axis in range(len(dims))])
    return factor_of


def normal_values(rng, shape, deviation, limit, cuts=(), held_as=jnp.bfloat16):
    entries = deviation * jax.random.normal(rng, shape, jnp.float32)
    if cuts:
        entries = entries * level_of(rng, shape, cuts, -0.22, 0.18)
    return jnp.clip(entries, -limit, limit).astype(held_as)


def setup_inputs(seed: int = 0, part: int = 0) -> dict:
    streams_of = jax.random.split(jax.random.key(seed), 17)
    part_keys = jax.random.split(jax.random.fold_in(streams_of[16], part), 17)
    tokens = normal_values(part_keys[0], (TOKENS, D), 1.0, 6.0, ((0, 4),))
    w_query = normal_values(streams_of[1], (D, HEADS * DK), D ** -0.5, 0.125, ((1, 4),))
    w_key = normal_values(streams_of[2], (D, HEADS * DK), D ** -0.5, 0.125, ((1, 4),))
    w_value = normal_values(streams_of[3], (D, HEADS * DV), D ** -0.5, 0.125, ((1, 4),))
    w_decay = normal_values(streams_of[4], (D, HEADS * DK), D ** -0.5, 0.125, ((1, 4),))
    decay_rate = draw_decay_rate(jax.random.fold_in(streams_of[16], 71), part)
    block_scale = jnp.clip(jnp.exp(math.log(2.0) - 1.3862944 * jax.random.uniform(part_keys[6], (TOKENS // BLK,), jnp.float32) ** level_of(part_keys[6], (TOKENS // BLK,), ((0, 4),), -0.2, 0.2)), 0.5, 2.0)
    w_rquery = normal_values(streams_of[7], (D, HEADS * DV), D ** -0.5, 0.125, ((1, 4),))
    w_gate = normal_values(streams_of[8], (D, HEADS * DV), D ** -0.5, 0.125, ((1, 4),))
    w_rkey = normal_values(streams_of[9], (D, HEADS * DV), D ** -0.5, 0.125, ((1, 4),))
    w_rvalue = normal_values(streams_of[10], (D, HEADS * DV), (max(1, D // 512)) ** -0.5, 3.0, ((1, 4),))
    query_gain = jnp.clip(1.0 + 0.18 * jax.random.normal(streams_of[11], (DV,), jnp.float32), 0.1, 1.9)
    key_gain = jnp.clip(1.0 + 0.18 * jax.random.normal(streams_of[12], (DV,), jnp.float32), 0.1, 1.9)
    out_gain = jnp.clip(1.0 + 0.18 * jax.random.normal(streams_of[13], (HEADS * DV,), jnp.float32), 0.1, 1.9)
    store = normal_values(part_keys[14], (PASSAGES, PLEN, D), 1.0, 6.0, ((0, 4),))
    passage_ids = draw_passage_ids(jax.random.fold_in(jax.random.fold_in(streams_of[16], part), 71), part)
    return dict(tokens=tokens, w_query=w_query, w_key=w_key, w_value=w_value, w_decay=w_decay, decay_rate=decay_rate, block_scale=block_scale, w_rquery=w_rquery, w_gate=w_gate, w_rkey=w_rkey, w_rvalue=w_rvalue, query_gain=query_gain, key_gain=key_gain, out_gain=out_gain, store=store, passage_ids=passage_ids)


EPS = 1e-06
PRECISE = lax.Precision.HIGHEST

def head_norm(values, gain_row):
    return values * lax.rsqrt(lax.optimization_barrier(jnp.mean(values * values, axis=-1, keepdims=True)) + EPS) * gain_row

def gla_blocks(gla_query, gla_key, gla_value, log_decay):
    head_dim = gla_query.shape[-1]
    block_len = gla_query.shape[1]
    cumulative = jnp.cumsum(log_decay, axis=1)
    query_dec = gla_query * head_dim ** (-0.5) * jnp.exp(cumulative)
    key_dec = gla_key * jnp.exp(-cumulative)
    causal_mask = jnp.arange(block_len)[:, None] >= jnp.arange(block_len)[None, :]
    scores = jnp.einsum('nihd,njhd->nhij', query_dec, key_dec, precision=PRECISE)
    scores = jnp.where(causal_mask, scores, 0.0)
    within = jnp.einsum('nhij,njhv->nihv', scores, gla_value, precision=PRECISE)
    block_total = cumulative[:, -1:]
    update = jnp.einsum('njhd,njhv->nhdv', gla_key * jnp.exp(block_total - cumulative), gla_value, precision=PRECISE)
    carry_decay = jnp.exp(block_total[:, 0])

    def advance(carry_state, block_item):
        query_part, state_delta, factor = block_item
        result = jnp.einsum('ihd,hdv->ihv', query_part, carry_state, precision=PRECISE)
        return (factor[..., None] * carry_state + state_delta, result)
    start_state = jnp.zeros((gla_query.shape[2], head_dim, gla_value.shape[-1]), jnp.float32)
    _, carried = lax.scan(advance, start_state, (query_dec, update, carry_decay))
    return within + carried

def reference(tokens, w_query, w_key, w_value, w_decay, decay_rate, block_scale, w_rquery, w_gate, w_rkey, w_rvalue, query_gain, key_gain, out_gain, store, passage_ids):
    seq_count = TOKENS // LEN
    gla_q = jnp.dot(tokens, w_query, preferred_element_type=jnp.float32)
    gla_k = jnp.dot(tokens, w_key, preferred_element_type=jnp.float32)
    gla_v = jnp.dot(tokens, w_value, preferred_element_type=jnp.float32)
    decay_pre = jnp.dot(tokens, w_decay, preferred_element_type=jnp.float32)
    log_decay = -2.0 * decay_rate[None, :] * jax.nn.sigmoid(decay_pre) * jnp.repeat(block_scale, BLK)[:, None]

    def shaped(values, width):
        return values.reshape(seq_count, LEN // BLK, BLK, HEADS, width)

    def one_sequence(seq_item):
        return gla_blocks(*seq_item)
    gla_out = lax.map(one_sequence, (shaped(gla_q, DK), shaped(gla_k, DK), shaped(gla_v, DV), shaped(log_decay, DK)))
    gla_out = gla_out.reshape(TOKENS, HEADS * DV)
    read_query = jnp.dot(tokens, w_rquery, preferred_element_type=jnp.float32).reshape(TOKENS, HEADS, DV)
    read_query = head_norm(read_query, query_gain).astype(jnp.bfloat16)
    read_query = read_query.reshape(TOKENS // BLK, BLK, HEADS, DV)

    def one_block(block_item):
        block_query, block_ids = block_item
        held_rows = jnp.take(store, block_ids.astype(jnp.int32), axis=0).reshape(NPASS * PLEN, D)
        passage_keys = jnp.dot(held_rows, w_rkey, preferred_element_type=jnp.float32).astype(jnp.bfloat16)
        passage_values = jnp.dot(held_rows, w_rvalue, preferred_element_type=jnp.float32).astype(jnp.bfloat16)
        key_normed = head_norm(passage_keys.astype(jnp.float32).reshape(NPASS * PLEN, HEADS, DV), key_gain).astype(jnp.bfloat16)
        scores = jnp.einsum('qhd,khd->hqk', block_query.astype(jnp.float32), key_normed.astype(jnp.float32), precision=PRECISE) * DV ** (-0.5)
        expd = jnp.exp(scores)
        read_weight = (expd / lax.optimization_barrier(jnp.sum(expd, axis=-1, keepdims=True))).astype(jnp.bfloat16)
        value_rows = passage_values.astype(jnp.float32).reshape(NPASS * PLEN, HEADS, DV)
        return jnp.einsum('hqk,khd->qhd', read_weight.astype(jnp.float32), value_rows, precision=PRECISE)
    retrieved = lax.map(one_block, (read_query, passage_ids)).reshape(TOKENS, HEADS * DV)
    gate_value = jax.nn.sigmoid(jnp.dot(tokens, w_gate, preferred_element_type=jnp.float32))
    combined = gla_out + gate_value * retrieved
    square_mean = lax.optimization_barrier(jnp.mean(combined * combined, axis=1, keepdims=True))
    return (combined * lax.rsqrt(square_mean + EPS) * out_gain[None, :]).astype(jnp.bfloat16)
```

```python
import functools

import jax
import jax.numpy as jnp
from jax import lax
from jax.experimental import pallas as pl
from jax.experimental.pallas import tpu as pltpu
from jax.sharding import PartitionSpec as P

HEADS = 8
DK = 64
DV = 128
BLK = 128
NPASS = 4
PAIR = 2
EPS = 1e-06
PRECISE = lax.Precision.HIGHEST
F32 = jnp.float32
BF16 = jnp.bfloat16
MESH = pl.DeviceIdType.MESH
NT = (((1,), (1,)), ((), ()))
TN = (((0,), (0,)), ((), ()))


def head_norm(values, gain_row):
    return values * lax.rsqrt(jnp.mean(values * values, axis=-1, keepdims=True) + EPS) * gain_row


def query_kernel(tok_ref, w_ref, gain_ref, out_ref):
    made = jnp.dot(tok_ref[...], w_ref[...], preferred_element_type=F32)
    for h in range(made.shape[1] // DV):
        cols = slice(h * DV, (h + 1) * DV)
        out_ref[:, cols] = head_norm(made[:, cols], gain_ref[...]).astype(BF16)


def passage_kernel(rows_ref, wk_ref, wv_ref, gain_ref, out_ref):
    rows = rows_ref[...]
    width = wk_ref.shape[1]
    keys = jnp.dot(rows, wk_ref[...], preferred_element_type=F32).astype(BF16).astype(F32)
    for h in range(width // DV):
        cols = slice(h * DV, (h + 1) * DV)
        out_ref[:, cols] = head_norm(keys[:, cols], gain_ref[...]).astype(BF16)
    out_ref[:, width:] = jnp.dot(rows, wv_ref[...], preferred_element_type=F32).astype(BF16)


def gla_kernel(
    scale_ref, tok_ref, rate_ref, wq, wk, wd, wv, wg, gla_ref, gate_ref, w_all, state, sems
):
    step = pl.program_id(0)
    dk = wq.shape[1]
    dv = wv.shape[1]

    @pl.when(step == 0)
    def _():
        copies = []
        at = 0
        for i, w in enumerate((wq, wk, wd, wv, wg)):
            copies.append(
                pltpu.make_async_copy(w, w_all.at[:, pl.ds(at, w.shape[1])], sems.at[i])
            )
            at += w.shape[1]
        for copy in copies:
            copy.start()
        state[...] = jnp.zeros_like(state)
        for copy in copies:
            copy.wait()

    made = jnp.dot(tok_ref[...], w_all[...], preferred_element_type=F32)
    gate_ref[...] = jax.nn.sigmoid(made[:, 3 * dk + dv :])
    row_id = lax.broadcasted_iota(jnp.int32, (BLK, BLK), 0)
    col_id = lax.broadcasted_iota(jnp.int32, (BLK, BLK), 1)
    causal = row_id >= col_id
    lower = causal.astype(F32)
    lane_head = lax.broadcasted_iota(jnp.int32, (BLK, dk), 1) // DK
    blocks = tok_ref.shape[0] // BLK
    for i in range(blocks):
        rows = slice(i * BLK, (i + 1) * BLK)
        q, k = made[rows, :dk], made[rows, dk : 2 * dk]
        pre, v = made[rows, 2 * dk : 3 * dk], made[rows, 3 * dk : 3 * dk + dv]
        block_scale = scale_ref[step * blocks + i]
        log_decay = -2.0 * rate_ref[...] * jax.nn.sigmoid(pre) * block_scale
        cum = jnp.dot(lower, log_decay, precision=PRECISE, preferred_element_type=F32)
        total = cum[BLK - 1 : BLK, :]
        q_dec = q * (DK ** (-0.5)) * jnp.exp(cum)
        k_dec = k * jnp.exp(-cum)
        k_up = k * jnp.exp(total - cum)
        held = state[...]
        for h in range(dv // DV):
            cols = slice(h * DV, (h + 1) * DV)
            q_h = jnp.where(lane_head == h, q_dec, 0.0)
            scores = lax.dot_general(q_h, k_dec, NT, precision=PRECISE, preferred_element_type=F32)
            scores = jnp.where(causal, scores, 0.0)
            gla_ref[rows, cols] = jnp.dot(
                scores, v[:, cols], precision=PRECISE, preferred_element_type=F32
            ) + lax.dot_general(q_h, held[cols], NT, precision=PRECISE, preferred_element_type=F32)
        state[...] = held * jnp.exp(total) + lax.dot_general(
            v, k_up, TN, precision=PRECISE, preferred_element_type=F32
        )


def read_kernel(reads, n_st, ids_ref, q_ref, own_ref, other_ref, num_ref, den_ref,
                kv, num_acc, den_acc, list_b, list_r, sems):
    held = own_ref.shape[0]
    width = q_ref.shape[2]
    copies = [
        pltpu.make_async_copy(own_ref, kv.at[pl.ds(0, held)], sems.at[0]),
        pltpu.make_async_copy(other_ref, kv.at[pl.ds(held, held)], sems.at[1]),
    ]
    for copy in copies:
        copy.start()
    me = lax.axis_index("st")
    chip = lax.div(me, PAIR)
    num_acc[...] = jnp.zeros_like(num_acc)
    den_acc[...] = jnp.zeros_like(den_acc)
    count = jnp.int32(0)
    for b in range(ids_ref.shape[0]):
        for j in range(ids_ref.shape[1]):
            name = ids_ref[b, j]
            owner = lax.div(name, held)
            row = name - owner * held
            list_b[count] = jnp.int32(b)
            list_r[count] = jnp.where(owner == me, row, row + held)
            count = count + jnp.where(lax.div(owner, PAIR) == chip, 1, 0)
    for copy in copies:
        copy.wait()
    ones = jnp.ones((8, kv.shape[1]), BF16)
    for r in range(reads):
        b, row = list_b[r], list_r[r]
        for h in range(width // DV):
            cols = slice(h * DV, (h + 1) * DV)
            score = lax.dot_general(
                q_ref[b, :, cols], kv[row, :, cols], NT, preferred_element_type=F32
            )
            expd = jnp.exp(score * (DV ** (-0.5))).astype(BF16)
            num_acc[b, :, cols] += jnp.dot(
                expd, kv[row, :, width + h * DV : width + (h + 1) * DV],
                preferred_element_type=F32,
            )
            den_acc[h, b] += lax.dot_general(ones, expd, NT, preferred_element_type=F32)
    num_ref[...] = num_acc[...].astype(BF16)
    for h in range(width // DV):
        for b in range(q_ref.shape[0]):
            den_ref[h, b : b + 1] = den_acc[h, b, 0:1]


def finish_kernel(parts, n_tp, *refs):
    gla_ref, gate_ref, gain_ref = refs[:3]
    nums, dens = refs[3 : 3 + parts], refs[3 + parts : 3 + 2 * parts]
    out_ref, combined, mine, theirs, send_sems, recv_sems = refs[3 + 2 * parts :]
    me = lax.axis_index("tp")
    barrier = pltpu.get_barrier_semaphore()
    peers = [lax.rem(me + k, n_tp) for k in range(1, n_tp)]
    for peer in peers:
        pl.semaphore_signal(barrier, inc=1, device_id={"tp": peer}, device_id_type=MESH)
    blocks, heads = mine.shape[0], dens[0].shape[0]
    width = out_ref.shape[1]
    inverse = []
    for h in range(heads):
        den = dens[0][h]
        for extra in dens[1:]:
            den = den + extra[h]
        inverse.append(jnp.transpose(1.0 / den, (1, 0)))
    ones = jnp.ones((8, width), F32)
    for b in range(blocks):
        rows = slice(b * BLK, (b + 1) * BLK)
        for h in range(heads):
            cols = slice(h * DV, (h + 1) * DV)
            num = nums[0][b, :, cols].astype(F32)
            for extra in nums[1:]:
                num = num + extra[b, :, cols].astype(F32)
            combined[rows, cols] = (
                gla_ref[rows, cols] + gate_ref[rows, cols] * (num * inverse[h][:, b : b + 1])
            )
        held = combined[rows, :]
        sums = lax.dot_general(ones, held * held, NT, precision=PRECISE, preferred_element_type=F32)
        mine[b : b + 1, :] = sums[0:1]
    pl.semaphore_wait(barrier, n_tp - 1)
    copies = []
    for k, peer in enumerate(peers):
        copies.append(
            pltpu.make_async_remote_copy(
                src_ref=mine,
                dst_ref=theirs.at[k],
                send_sem=send_sems.at[k],
                recv_sem=recv_sems.at[k],
                device_id={"tp": peer},
                device_id_type=MESH,
            )
        )
    for copy in copies:
        copy.start()
    for copy in copies:
        copy.wait()
    total = mine[...]
    for k in range(n_tp - 1):
        total = total + theirs[k]
    scale = jnp.transpose(lax.rsqrt(total / (HEADS * DV) + EPS), (1, 0))
    for b in range(blocks):
        rows = slice(b * BLK, (b + 1) * BLK)
        out_ref[rows, :] = (combined[rows, :] * scale[:, b : b + 1] * gain_ref[...]).astype(BF16)


def cost(flops, moved):
    return pl.CostEstimate(flops=int(flops), bytes_accessed=int(moved), transcendentals=0)


def on_device(n_st, n_tp, tokens, w_query, w_key, w_value, w_decay, decay_rate, block_scale,
              w_rquery, w_gate, w_rkey, w_rvalue, query_gain, key_gain, out_gain, store,
              passage_ids):
    length, depth = tokens.shape
    num_blocks = length // BLK
    width = w_value.shape[1]
    heads = width // DV
    stores_here, passage_rows, _ = store.shape
    tile = 2 * BLK
    whole = lambda *shape: pl.BlockSpec(shape, lambda i, *_: (0,) * len(shape))
    any_spec = pl.BlockSpec(memory_space=pl.ANY)
    vmem = pl.BlockSpec(memory_space=pltpu.VMEM)

    def shift(values, by):
        return lax.ppermute(values, "st", [(s, (s + by) % n_st) for s in range(n_st)])

    read_query = pl.pallas_call(
        query_kernel,
        grid=(length // tile,),
        in_specs=[
            pl.BlockSpec((tile, depth), lambda i: (i, 0)),
            whole(depth, width),
            whole(1, DV),
        ],
        out_specs=pl.BlockSpec((tile, width), lambda i: (i, 0)),
        out_shape=jax.ShapeDtypeStruct((length, width), BF16),
        cost_estimate=cost(2 * length * depth * width, 6e6),
        name="query",
    )(tokens, w_rquery, query_gain.reshape(1, DV)).reshape(num_blocks, BLK, width)

    groups = range(1, n_st // PAIR)
    queries = [read_query] + [shift(read_query, PAIR * k) for k in groups]
    ids = [passage_ids] + [shift(passage_ids, PAIR * k) for k in groups]

    rows = stores_here * passage_rows
    made = pl.pallas_call(
        passage_kernel,
        grid=(rows // tile,),
        in_specs=[
            pl.BlockSpec((tile, depth), lambda i: (i, 0)),
            whole(depth, width),
            whole(depth, width),
            whole(1, DV),
        ],
        out_specs=pl.BlockSpec((tile, 2 * width), lambda i: (i, 0)),
        out_shape=jax.ShapeDtypeStruct((rows, 2 * width), BF16),
        cost_estimate=cost(4 * rows * depth * width, 1e7),
        name="passages",
    )(store.reshape(rows, depth), w_rkey, w_rvalue, key_gain.reshape(1, DV))
    made = made.reshape(stores_here, passage_rows, 2 * width)
    other = lax.ppermute(made, "st", [(s, s ^ 1) for s in range(n_st)])

    request_count = passage_ids.shape[0] * passage_ids.shape[1]
    most = request_count // min(n_st, request_count // 2)
    nums, dens = [], []
    for k, (query, names) in enumerate(zip(queries, ids)):
        num, den = pl.pallas_call(
            functools.partial(read_kernel, PAIR * most, n_st),
            in_specs=[
                pl.BlockSpec(memory_space=pltpu.SMEM), vmem, any_spec, any_spec,
            ],
            out_specs=[vmem, vmem],
            out_shape=[
                jax.ShapeDtypeStruct((num_blocks, BLK, width), BF16),
                jax.ShapeDtypeStruct((heads, num_blocks, BLK), F32),
            ],
            scratch_shapes=[
                pltpu.VMEM((2 * stores_here, passage_rows, 2 * width), BF16),
                pltpu.VMEM((num_blocks, BLK, width), F32),
                pltpu.VMEM((heads, num_blocks, 8, BLK), F32),
                pltpu.SMEM((request_count + 1,), jnp.int32),
                pltpu.SMEM((request_count + 1,), jnp.int32),
                pltpu.SemaphoreType.DMA((2,)),
            ],
            cost_estimate=cost(2e9, 5e6),
            name="reads",
        )(names, query, made, other)
        if k:
            num, den = shift(num, -PAIR * k), shift(den, -PAIR * k)
        nums.append(num)
        dens.append(den)

    spare = -w_query.shape[1] % BLK
    if spare:
        w_query, w_key, w_decay = (
            jnp.pad(w, ((0, 0), (0, spare))) for w in (w_query, w_key, w_decay)
        )
        decay_rate = jnp.pad(decay_rate, (0, spare))
    dk = w_query.shape[1]
    gla_out, gate = pl.pallas_call(
        gla_kernel,
        grid=(length // tile,),
        in_specs=[
            pl.BlockSpec(memory_space=pltpu.SMEM),
            pl.BlockSpec((tile, depth), lambda i: (i, 0)),
            whole(1, dk),
        ]
        + [any_spec] * 5,
        out_specs=[pl.BlockSpec((tile, width), lambda i: (i, 0))] * 2,
        out_shape=[jax.ShapeDtypeStruct((length, width), F32)] * 2,
        scratch_shapes=[
            pltpu.VMEM((depth, 3 * dk + 2 * width), BF16),
            pltpu.VMEM((width, dk), F32),
            pltpu.SemaphoreType.DMA((5,)),
        ],
        cost_estimate=cost(8e9, 1e7),
        name="gla",
    )(block_scale, tokens, decay_rate.reshape(1, dk), w_query, w_key, w_decay, w_value, w_gate)

    return pl.pallas_call(
        functools.partial(finish_kernel, len(nums), n_tp),
        in_specs=[vmem] * (3 + 2 * len(nums)),
        out_specs=vmem,
        out_shape=jax.ShapeDtypeStruct((length, width), BF16),
        scratch_shapes=[
            pltpu.VMEM((length, width), F32),
            pltpu.VMEM((num_blocks, BLK), F32),
            pltpu.VMEM((max(n_tp - 1, 1), num_blocks, BLK), F32),
            pltpu.SemaphoreType.DMA((max(n_tp - 1, 1),)),
            pltpu.SemaphoreType.DMA((max(n_tp - 1, 1),)),
        ],
        compiler_params=pltpu.CompilerParams(collective_id=0, has_side_effects=True),
        cost_estimate=cost(1e9, 6e6),
        name="finish",
    )(gla_out, gate, out_gain.reshape(1, width), *nums, *dens)


def solution(mesh):
    return jax.shard_map(
        functools.partial(on_device, mesh.shape["st"], mesh.shape["tp"]),
        mesh=mesh,
        in_specs=(
            P(("grp", "st"), None),
            P(None, "tp"),
            P(None, "tp"),
            P(None, "tp"),
            P(None, "tp"),
            P("tp"),
            P(("grp", "st")),
            P(None, "tp"),
            P(None, "tp"),
            P(None, "tp"),
            P(None, "tp"),
            P(),
            P(),
            P("tp"),
            P(("grp", "st"), None, None),
            P(("grp", "st"), None),
        ),
        out_specs=P(("grp", "st"), "tp"),
        check_vma=False,
    )
```

```python
import functools

import jax
import jax.numpy as jnp
from jax import lax
from jax.experimental import pallas as pl
from jax.experimental.pallas import tpu as pltpu
from jax.sharding import PartitionSpec as P


HEADS = 8
DK = 64
DV = 128
BLK = 128
PAIR = 2
EPS = 1e-06
F32 = jnp.float32
BF16 = jnp.bfloat16
MESH = pl.DeviceIdType.MESH
NT = (((1,), (1,)), ((), ()))
TN = (((0,), (0,)), ((), ()))


def head_norm(values, gain_row):
    return values * lax.rsqrt(jnp.mean(values * values, axis=-1, keepdims=True) + EPS) * gain_row


def split(values):
    high = values.astype(BF16)
    return high, (values - high.astype(F32)).astype(BF16)


def query_kernel(tok_ref, w_ref, gain_ref, out_ref):
    made = jnp.dot(tok_ref[...], w_ref[...], preferred_element_type=F32)
    for h in range(made.shape[1] // DV):
        cols = slice(h * DV, (h + 1) * DV)
        out_ref[:, cols] = head_norm(made[:, cols], gain_ref[...]).astype(BF16)


def passage_kernel(rows_ref, wk_ref, wv_ref, gain_ref, out_ref):
    rows = rows_ref[...]
    width = wk_ref.shape[1]
    keys = jnp.dot(rows, wk_ref[...], preferred_element_type=F32).astype(BF16).astype(F32)
    for h in range(width // DV):
        cols = slice(h * DV, (h + 1) * DV)
        out_ref[:, cols] = head_norm(keys[:, cols], gain_ref[...]).astype(BF16)
    out_ref[:, width:] = jnp.dot(rows, wv_ref[...], preferred_element_type=F32).astype(BF16)


def gla_kernel(
    scale_ref, tok_ref, rate_ref, wq, wk, wd, wv, wg, gla_ref, gate_ref, w_all, state, sems
):
    step = pl.program_id(0)
    dk = wq.shape[1]
    dv = wv.shape[1]

    @pl.when(step == 0)
    def _():
        copies = []
        at = 0
        for i, w in enumerate((wq, wk, wd, wv, wg)):
            copies.append(
                pltpu.make_async_copy(w, w_all.at[:, pl.ds(at, w.shape[1])], sems.at[i])
            )
            at += w.shape[1]
        for copy in copies:
            copy.start()
        state[...] = jnp.zeros_like(state)
        for copy in copies:
            copy.wait()

    made = jnp.dot(tok_ref[...], w_all[...], preferred_element_type=F32)
    gate_ref[...] = jax.nn.sigmoid(made[:, 3 * dk + dv :])
    row_id = lax.broadcasted_iota(jnp.int32, (BLK, BLK), 0)
    col_id = lax.broadcasted_iota(jnp.int32, (BLK, BLK), 1)
    causal = row_id >= col_id
    lower = causal.astype(F32)
    lower = jnp.concatenate([lower, lower], axis=1).astype(BF16)
    lane_head = lax.broadcasted_iota(jnp.int32, (BLK, dk), 1) // DK
    blocks = tok_ref.shape[0] // BLK
    for i in range(blocks):
        rows = slice(i * BLK, (i + 1) * BLK)
        q, k = made[rows, :dk], made[rows, dk : 2 * dk]
        pre, v = made[rows, 2 * dk : 3 * dk], made[rows, 3 * dk : 3 * dk + dv]
        block_scale = scale_ref[step * blocks + i]
        log_decay = -2.0 * rate_ref[...] * jax.nn.sigmoid(pre) * block_scale
        high, low = split(log_decay)
        cum = jnp.dot(
            lower, jnp.concatenate([high, low], axis=0), preferred_element_type=F32
        )
        total = cum[BLK - 1 : BLK, :]
        k_dec = k * jnp.exp(-cum)
        q_high, q_low = split(q * (DK ** (-0.5)) * jnp.exp(cum))
        k_high, k_low = split(k_dec)
        k_twice = jnp.concatenate([k_high, k_high], axis=1)
        up = jnp.concatenate(split(k * jnp.exp(total - cum)), axis=1)
        v_high = v.astype(BF16)
        v_twice = jnp.concatenate([v_high, v_high], axis=0)
        held = state[...]
        held_high = held.astype(BF16)
        held_twice = jnp.concatenate([held_high, held_high], axis=1)
        for h in range(dv // DV):
            cols = slice(h * DV, (h + 1) * DV)
            mine = lane_head == h
            zero = jnp.zeros((), BF16)
            own_high = jnp.where(mine, q_high, zero)
            q_h = jnp.concatenate([own_high, jnp.where(mine, q_low, zero)], axis=1)
            scores = lax.dot_general(
                q_h, k_twice, NT, preferred_element_type=F32
            ) + lax.dot_general(own_high, k_low, NT, preferred_element_type=F32)
            scores = jnp.concatenate(split(jnp.where(causal, scores, 0.0)), axis=1)
            gla_ref[rows, cols] = jnp.dot(
                scores, v_twice[:, cols], preferred_element_type=F32
            ) + lax.dot_general(q_h, held_twice[cols], NT, preferred_element_type=F32)
        added = lax.dot_general(v_high, up, TN, preferred_element_type=F32)
        state[...] = held * jnp.exp(total) + added[:, :dk] + added[:, dk:]


def read_kernel(reads, ids_ref, q_ref, own_ref, other_ref, num_ref, den_ref,
                kv, num_acc, den_acc, list_b, list_r, sems):
    held = own_ref.shape[0]
    width = q_ref.shape[2]
    copies = [
        pltpu.make_async_copy(own_ref, kv.at[pl.ds(0, held)], sems.at[0]),
        pltpu.make_async_copy(other_ref, kv.at[pl.ds(held, held)], sems.at[1]),
    ]
    for copy in copies:
        copy.start()
    me = lax.axis_index("st")
    chip = lax.div(me, PAIR)
    num_acc[...] = jnp.zeros_like(num_acc)
    den_acc[...] = jnp.zeros_like(den_acc)
    count = jnp.int32(0)
    for b in range(ids_ref.shape[0]):
        for j in range(ids_ref.shape[1]):
            name = ids_ref[b, j]
            owner = lax.div(name, held)
            row = name - owner * held
            list_b[count] = jnp.int32(b)
            list_r[count] = jnp.where(owner == me, row, row + held)
            count = count + jnp.where(lax.div(owner, PAIR) == chip, 1, 0)
    for copy in copies:
        copy.wait()
    ones = jnp.ones((8, kv.shape[1]), BF16)
    group = 4 if reads % 4 == 0 else 1
    heads = [(h, slice(h * DV, (h + 1) * DV)) for h in range(width // DV)]
    for first in range(0, reads, group):
        items = []
        for r in range(first, first + group):
            b, row = list_b[r], list_r[r]
            for h, cols in heads:
                score = lax.dot_general(
                    q_ref[b, :, cols], kv[row, :, cols], NT, preferred_element_type=F32
                )
                items.append((b, row, h, cols, score))
        exps = [jnp.exp(item[-1] * (DV ** (-0.5))).astype(BF16) for item in items]
        made = []
        for (b, row, h, cols, _), expd in zip(items, exps):
            value = kv[row, :, width + h * DV : width + (h + 1) * DV]
            made.append((
                jnp.dot(expd, value, preferred_element_type=F32),
                lax.dot_general(ones, expd, NT, preferred_element_type=F32),
            ))
        for (b, row, h, cols, _), (num, den) in zip(items, made):
            num_acc[b, :, cols] += num
            den_acc[h, b] += den
    num_ref[...] = num_acc[...].astype(BF16)
    for h in range(width // DV):
        for b in range(q_ref.shape[0]):
            den_ref[h, b : b + 1] = den_acc[h, b, 0:1]


def finish_kernel(parts, n_tp, *refs):
    gla_ref, gate_ref, gain_ref = refs[:3]
    nums, dens = refs[3 : 3 + parts], refs[3 + parts : 3 + 2 * parts]
    out_ref, combined, mine, theirs, send_sems, recv_sems = refs[3 + 2 * parts :]
    me = lax.axis_index("tp")
    barrier = pltpu.get_barrier_semaphore()
    peers = [lax.rem(me + k, n_tp) for k in range(1, n_tp)]
    for peer in peers:
        pl.semaphore_signal(barrier, inc=1, device_id={"tp": peer}, device_id_type=MESH)
    blocks, heads = mine.shape[0], dens[0].shape[0]
    width = out_ref.shape[1]
    inverse = []
    for h in range(heads):
        den = dens[0][h]
        for extra in dens[1:]:
            den = den + extra[h]
        inverse.append(jnp.transpose(1.0 / den, (1, 0)))
    ones = jnp.ones((8, 2 * width), BF16)
    for b in range(blocks):
        rows = slice(b * BLK, (b + 1) * BLK)
        for h in range(heads):
            cols = slice(h * DV, (h + 1) * DV)
            num = nums[0][b, :, cols].astype(F32)
            for extra in nums[1:]:
                num = num + extra[b, :, cols].astype(F32)
            combined[rows, cols] = (
                gla_ref[rows, cols] + gate_ref[rows, cols] * (num * inverse[h][:, b : b + 1])
            )
        held = combined[rows, :]
        sums = lax.dot_general(
            ones, jnp.concatenate(split(held * held), axis=1), NT, preferred_element_type=F32
        )
        mine[b : b + 1, :] = sums[0:1]
    pl.semaphore_wait(barrier, n_tp - 1)
    copies = []
    for k, peer in enumerate(peers):
        copies.append(
            pltpu.make_async_remote_copy(
                src_ref=mine,
                dst_ref=theirs.at[k],
                send_sem=send_sems.at[k],
                recv_sem=recv_sems.at[k],
                device_id={"tp": peer},
                device_id_type=MESH,
            )
        )
    for copy in copies:
        copy.start()
    for copy in copies:
        copy.wait()
    total = mine[...]
    for k in range(n_tp - 1):
        total = total + theirs[k]
    scale = jnp.transpose(lax.rsqrt(total / (HEADS * DV) + EPS), (1, 0))
    for b in range(blocks):
        rows = slice(b * BLK, (b + 1) * BLK)
        out_ref[rows, :] = (combined[rows, :] * scale[:, b : b + 1] * gain_ref[...]).astype(BF16)


def cost(flops, moved):
    return pl.CostEstimate(flops=int(flops), bytes_accessed=int(moved), transcendentals=0)


def on_device(n_st, n_tp, tokens, w_query, w_key, w_value, w_decay, decay_rate, block_scale,
              w_rquery, w_gate, w_rkey, w_rvalue, query_gain, key_gain, out_gain, store,
              passage_ids):
    length, depth = tokens.shape
    num_blocks = length // BLK
    width = w_value.shape[1]
    heads = width // DV
    stores_here, passage_rows, _ = store.shape
    tile = 2 * BLK
    tall = 4 * BLK
    whole = lambda *shape: pl.BlockSpec(shape, lambda i, *_: (0,) * len(shape))
    any_spec = pl.BlockSpec(memory_space=pl.ANY)
    vmem = pl.BlockSpec(memory_space=pltpu.VMEM)

    def shift(values, by):
        return lax.ppermute(values, "st", [(s, (s + by) % n_st) for s in range(n_st)])

    read_query = pl.pallas_call(
        query_kernel,
        grid=(length // tall,),
        in_specs=[
            pl.BlockSpec((tall, depth), lambda i: (i, 0)),
            whole(depth, width),
            whole(1, DV),
        ],
        out_specs=pl.BlockSpec((tall, width), lambda i: (i, 0)),
        out_shape=jax.ShapeDtypeStruct((length, width), BF16),
        cost_estimate=cost(2 * length * depth * width, 6e6),
        name="query",
    )(tokens, w_rquery, query_gain.reshape(1, DV)).reshape(num_blocks, BLK, width)

    groups = range(1, n_st // PAIR)
    queries = [read_query] + [shift(read_query, PAIR * k) for k in groups]
    ids = [passage_ids] + [shift(passage_ids, PAIR * k) for k in groups]

    held_store, _ = lax.optimization_barrier((store, read_query))
    rows = stores_here * passage_rows
    made = pl.pallas_call(
        passage_kernel,
        grid=(rows // tall,),
        in_specs=[
            pl.BlockSpec((tall, depth), lambda i: (i, 0)),
            whole(depth, width),
            whole(depth, width),
            whole(1, DV),
        ],
        out_specs=pl.BlockSpec((tall, 2 * width), lambda i: (i, 0)),
        out_shape=jax.ShapeDtypeStruct((rows, 2 * width), BF16),
        cost_estimate=cost(4 * rows * depth * width, 1e7),
        name="passages",
    )(held_store.reshape(rows, depth), w_rkey, w_rvalue, key_gain.reshape(1, DV))
    made = made.reshape(stores_here, passage_rows, 2 * width)
    other = lax.ppermute(made, "st", [(s, s ^ 1) for s in range(n_st)])

    request_count = passage_ids.shape[0] * passage_ids.shape[1]
    most = request_count // min(n_st, request_count // 2)

    def read(names, query):
        return pl.pallas_call(
            functools.partial(read_kernel, PAIR * most),
            in_specs=[
                pl.BlockSpec(memory_space=pltpu.SMEM), vmem, any_spec, any_spec,
            ],
            out_specs=[vmem, vmem],
            out_shape=[
                jax.ShapeDtypeStruct((num_blocks, BLK, width), BF16),
                jax.ShapeDtypeStruct((heads, num_blocks, BLK), F32),
            ],
            scratch_shapes=[
                pltpu.VMEM((2 * stores_here, passage_rows, 2 * width), BF16),
                pltpu.VMEM((num_blocks, BLK, width), F32),
                pltpu.VMEM((heads, num_blocks, 8, BLK), F32),
                pltpu.SMEM((request_count + 1,), jnp.int32),
                pltpu.SMEM((request_count + 1,), jnp.int32),
                pltpu.SemaphoreType.DMA((2,)),
            ],
            cost_estimate=cost(2e9, 5e6),
            name="reads",
        )(names, query, made, other)

    nums, dens = [], []
    for k in groups:
        num, den = read(ids[k], queries[k])
        tokens, _ = lax.optimization_barrier((tokens, num))
        nums.append(shift(num, -PAIR * k))
        dens.append(shift(den, -PAIR * k))

    spare = -w_query.shape[1] % BLK
    if spare:
        w_query, w_key, w_decay = (
            jnp.pad(w, ((0, 0), (0, spare))) for w in (w_query, w_key, w_decay)
        )
        decay_rate = jnp.pad(decay_rate, (0, spare))
    dk = w_query.shape[1]
    gla_out, gate = pl.pallas_call(
        gla_kernel,
        grid=(length // tile,),
        in_specs=[
            pl.BlockSpec(memory_space=pltpu.SMEM),
            pl.BlockSpec((tile, depth), lambda i: (i, 0)),
            whole(1, dk),
        ]
        + [any_spec] * 5,
        out_specs=[pl.BlockSpec((tile, width), lambda i: (i, 0))] * 2,
        out_shape=[jax.ShapeDtypeStruct((length, width), F32)] * 2,
        scratch_shapes=[
            pltpu.VMEM((depth, 3 * dk + 2 * width), BF16),
            pltpu.VMEM((width, dk), F32),
            pltpu.SemaphoreType.DMA((5,)),
        ],
        cost_estimate=cost(8e9, 1e7),
        name="gla",
    )(block_scale, tokens, decay_rate.reshape(1, dk), w_query, w_key, w_decay, w_value, w_gate)

    read_query, gla_out = lax.optimization_barrier((read_query, gla_out))
    num, den = read(passage_ids, read_query)
    nums.append(num)
    dens.append(den)

    return pl.pallas_call(
        functools.partial(finish_kernel, len(nums), n_tp),
        in_specs=[vmem] * (3 + 2 * len(nums)),
        out_specs=vmem,
        out_shape=jax.ShapeDtypeStruct((length, width), BF16),
        scratch_shapes=[
            pltpu.VMEM((length, width), F32),
            pltpu.VMEM((num_blocks, BLK), F32),
            pltpu.VMEM((max(n_tp - 1, 1), num_blocks, BLK), F32),
            pltpu.SemaphoreType.DMA((max(n_tp - 1, 1),)),
            pltpu.SemaphoreType.DMA((max(n_tp - 1, 1),)),
        ],
        compiler_params=pltpu.CompilerParams(collective_id=0, has_side_effects=True),
        cost_estimate=cost(1e9, 6e6),
        name="finish",
    )(gla_out, gate, out_gain.reshape(1, width), *nums, *dens)


def solution(mesh):
    def body(*args):
        return on_device(mesh.shape["st"], mesh.shape["tp"], *args)

    return jax.shard_map(
        body,
        mesh=mesh,
        in_specs=(
            P(("grp", "st"), None),
            P(None, "tp"),
            P(None, "tp"),
            P(None, "tp"),
            P(None, "tp"),
            P("tp"),
            P(("grp", "st")),
            P(None, "tp"),
            P(None, "tp"),
            P(None, "tp"),
            P(None, "tp"),
            P(),
            P(),
            P("tp"),
            P(("grp", "st"), None, None),
            P(("grp", "st"), None),
        ),
        out_specs=P(("grp", "st"), "tp"),
        check_vma=False,
    )
```

```python
import functools

import jax
import jax.numpy as jnp
from jax import lax
from jax.experimental import pallas as pl
from jax.experimental.pallas import tpu as pltpu
from jax.sharding import PartitionSpec as P


HEADS = 8
DK = 64
DV = 128
BLK = 128
PAIR = 2
EPS = 1e-06
F32 = jnp.float32
BF16 = jnp.bfloat16
MESH = pl.DeviceIdType.MESH
NT = (((1,), (1,)), ((), ()))
TN = (((0,), (0,)), ((), ()))


def head_norm(values, gain_row):
    return values * lax.rsqrt(jnp.mean(values * values, axis=-1, keepdims=True) + EPS) * gain_row


def split(values):
    high = values.astype(BF16)
    return high, (values - high.astype(F32)).astype(BF16)


def query_kernel(tok_ref, w_ref, gain_ref, out_ref):
    made = jnp.dot(tok_ref[...], w_ref[...], preferred_element_type=F32)
    for h in range(made.shape[1] // DV):
        cols = slice(h * DV, (h + 1) * DV)
        out_ref[:, cols] = head_norm(made[:, cols], gain_ref[...]).astype(BF16)


def passage_kernel(rows_ref, wk_ref, wv_ref, gain_ref, out_ref):
    rows = rows_ref[...]
    width = wk_ref.shape[1]
    keys = jnp.dot(rows, wk_ref[...], preferred_element_type=F32).astype(BF16).astype(F32)
    for h in range(width // DV):
        cols = slice(h * DV, (h + 1) * DV)
        out_ref[:, cols] = head_norm(keys[:, cols], gain_ref[...]).astype(BF16)
    out_ref[:, width:] = jnp.dot(rows, wv_ref[...], preferred_element_type=F32).astype(BF16)


def gla_kernel(
    first, scale_ref, tok_ref, rate_ref, given, wq, wk, wd, wv, wg,
    gla_ref, gate_ref, kept, w_all, state, sems
):
    step = pl.program_id(0)
    dk = wq.shape[1]
    dv = wv.shape[1]

    @pl.when(step == 0)
    def _():
        copies = []
        at = 0
        for i, w in enumerate((wq, wk, wd, wv, wg)):
            copies.append(
                pltpu.make_async_copy(w, w_all.at[:, pl.ds(at, w.shape[1])], sems.at[i])
            )
            at += w.shape[1]
        for copy in copies:
            copy.start()
        state[...] = given[...]
        for copy in copies:
            copy.wait()

    made = jnp.dot(tok_ref[...], w_all[...], preferred_element_type=F32)
    gate_ref[...] = jax.nn.sigmoid(made[:, 3 * dk + dv :])
    row_id = lax.broadcasted_iota(jnp.int32, (BLK, BLK), 0)
    col_id = lax.broadcasted_iota(jnp.int32, (BLK, BLK), 1)
    causal = row_id >= col_id
    lower = causal.astype(F32)
    lower = jnp.concatenate([lower, lower], axis=1).astype(BF16)
    lane_head = lax.broadcasted_iota(jnp.int32, (BLK, dk), 1) // DK
    zero = jnp.zeros((), BF16)
    blocks = tok_ref.shape[0] // BLK
    spans = [slice(i * BLK, (i + 1) * BLK) for i in range(blocks)]
    heads = [slice(h * DV, (h + 1) * DV) for h in range(dv // DV)]
    cums = []
    for i, rows in enumerate(spans):
        pre = made[rows, 2 * dk : 3 * dk]
        block_scale = scale_ref[first + step * blocks + i]
        high, low = split(-2.0 * rate_ref[...] * jax.nn.sigmoid(pre) * block_scale)
        cums.append(
            jnp.dot(lower, jnp.concatenate([high, low], axis=0), preferred_element_type=F32)
        )
    queries, scores, ups, totals, values = [], [], [], [], []
    for rows, cum in zip(spans, cums):
        q, k = made[rows, :dk], made[rows, dk : 2 * dk]
        total = cum[BLK - 1 : BLK, :]
        totals.append(jnp.exp(total))
        q_high, q_low = split(q * (DK ** (-0.5)) * jnp.exp(cum))
        k_high, k_low = split(k * jnp.exp(-cum))
        k_twice = jnp.concatenate([k_high, k_high], axis=1)
        ups.append(split(k * jnp.exp(total - cum)))
        values.append(split(made[rows, 3 * dk : 3 * dk + dv]))
        for h in range(len(heads)):
            own_high = jnp.where(lane_head == h, q_high, zero)
            own_low = jnp.where(lane_head == h, q_low, zero)
            q_h = jnp.concatenate([own_high, own_low], axis=1)
            queries.append(q_h)
            scores.append(
                lax.dot_general(q_h, k_twice, NT, preferred_element_type=F32)
                + lax.dot_general(own_high, k_low, NT, preferred_element_type=F32)
            )
    within, added = [], []
    for i in range(blocks):
        v_high, v_low = values[i]
        v_twice = jnp.concatenate([v_high, v_high], axis=0)
        for h, cols in enumerate(heads):
            high, low = split(jnp.where(causal, scores[i * len(heads) + h], 0.0))
            within.append(
                jnp.dot(
                    jnp.concatenate([high, low], axis=1),
                    v_twice[:, cols],
                    preferred_element_type=F32,
                )
                + jnp.dot(high, v_low[:, cols], preferred_element_type=F32)
            )
        up_high, up_low = ups[i]
        both = lax.dot_general(
            v_high, jnp.concatenate([up_high, up_low], axis=1), TN, preferred_element_type=F32
        )
        added.append(
            both[:, :dk]
            + both[:, dk:]
            + lax.dot_general(v_low, up_high, TN, preferred_element_type=F32)
        )
    held = state[...]
    for i, rows in enumerate(spans):
        held_high = held.astype(BF16)
        held_twice = jnp.concatenate([held_high, held_high], axis=1)
        for h, cols in enumerate(heads):
            n = i * len(heads) + h
            gla_ref[rows, cols] = within[n] + lax.dot_general(
                queries[n], held_twice[cols], NT, preferred_element_type=F32
            )
        held = held * totals[i] + added[i]
    state[...] = held
    kept[...] = held


def read_kernel(reads, ids_ref, q_ref, own_ref, other_ref, num_ref, den_ref,
                kv, num_acc, den_acc, list_b, list_r, sems):
    held = own_ref.shape[0]
    width = q_ref.shape[2]
    copies = [
        pltpu.make_async_copy(own_ref, kv.at[pl.ds(0, held)], sems.at[0]),
        pltpu.make_async_copy(other_ref, kv.at[pl.ds(held, held)], sems.at[1]),
    ]
    for copy in copies:
        copy.start()
    me = lax.axis_index("st")
    chip = lax.div(me, PAIR)
    num_acc[...] = jnp.zeros_like(num_acc)
    den_acc[...] = jnp.zeros_like(den_acc)
    count = jnp.int32(0)
    for b in range(ids_ref.shape[0]):
        for j in range(ids_ref.shape[1]):
            name = ids_ref[b, j]
            owner = lax.div(name, held)
            row = name - owner * held
            list_b[count] = jnp.int32(b)
            list_r[count] = jnp.where(owner == me, row, row + held)
            count = count + jnp.where(lax.div(owner, PAIR) == chip, 1, 0)
    for copy in copies:
        copy.wait()
    ones = jnp.ones((8, kv.shape[1]), BF16)
    group = 4 if reads % 4 == 0 else 1
    heads = [(h, slice(h * DV, (h + 1) * DV)) for h in range(width // DV)]
    for first in range(0, reads, group):
        items = []
        for r in range(first, first + group):
            b, row = list_b[r], list_r[r]
            for h, cols in heads:
                score = lax.dot_general(
                    q_ref[b, :, cols], kv[row, :, cols], NT, preferred_element_type=F32
                )
                items.append((b, row, h, cols, score))
        exps = [jnp.exp(item[-1] * (DV ** (-0.5))).astype(BF16) for item in items]
        made = []
        for (b, row, h, cols, _), expd in zip(items, exps):
            value = kv[row, :, width + h * DV : width + (h + 1) * DV]
            made.append((
                jnp.dot(expd, value, preferred_element_type=F32),
                lax.dot_general(ones, expd, NT, preferred_element_type=F32),
            ))
        for (b, row, h, cols, _), (num, den) in zip(items, made):
            num_acc[b, :, cols] += num
            den_acc[h, b] += den
    num_ref[...] = num_acc[...].astype(BF16)
    for h in range(width // DV):
        for b in range(q_ref.shape[0]):
            den_ref[h, b : b + 1] = den_acc[h, b, 0:1]


def finish_kernel(parts, n_tp, *refs):
    gain_ref, gla_parts, gate_parts = refs[0], refs[1:3], refs[3:5]
    refs = refs[5:]
    far, dens = refs[:parts], refs[parts : 2 * parts]
    (out_ref, gla_ref, gate_ref, *nums) = refs[2 * parts : 3 * parts + 3]
    combined, mine, theirs, send_sems, recv_sems, sems = refs[3 * parts + 3 :]
    blocks = mine.shape[0]
    half = blocks // 2
    loads = []
    for b in range(blocks):
        there, here = pl.ds(b % half * BLK, BLK), pl.ds(b * BLK, BLK)
        row = [
            pltpu.make_async_copy(gla_parts[b // half].at[there], gla_ref.at[here], sems.at[0, b]),
            pltpu.make_async_copy(gate_parts[b // half].at[there], gate_ref.at[here], sems.at[1, b]),
        ]
        for i in range(parts):
            row.append(pltpu.make_async_copy(far[i].at[b], nums[i].at[b], sems.at[2 + i, b]))
        for copy in row:
            copy.start()
        loads.append(row)
    me = lax.axis_index("tp")
    barrier = pltpu.get_barrier_semaphore()
    peers = [lax.rem(me + k, n_tp) for k in range(1, n_tp)]
    for peer in peers:
        pl.semaphore_signal(barrier, inc=1, device_id={"tp": peer}, device_id_type=MESH)
    heads = dens[0].shape[0]
    width = out_ref.shape[1]
    inverse = []
    for h in range(heads):
        den = dens[0][h]
        for extra in dens[1:]:
            den = den + extra[h]
        inverse.append(jnp.transpose(1.0 / den, (1, 0)))
    ones = jnp.ones((8, 2 * width), BF16)
    for b in range(blocks):
        rows = slice(b * BLK, (b + 1) * BLK)
        for copy in loads[b]:
            copy.wait()
        for h in range(heads):
            cols = slice(h * DV, (h + 1) * DV)
            num = nums[0][b, :, cols].astype(F32)
            for extra in nums[1:]:
                num = num + extra[b, :, cols].astype(F32)
            combined[rows, cols] = (
                gla_ref[rows, cols] + gate_ref[rows, cols] * (num * inverse[h][:, b : b + 1])
            )
        held = combined[rows, :]
        sums = lax.dot_general(
            ones, jnp.concatenate(split(held * held), axis=1), NT, preferred_element_type=F32
        )
        mine[b : b + 1, :] = sums[0:1]
    pl.semaphore_wait(barrier, n_tp - 1)
    copies = []
    for k, peer in enumerate(peers):
        copies.append(
            pltpu.make_async_remote_copy(
                src_ref=mine,
                dst_ref=theirs.at[k],
                send_sem=send_sems.at[k],
                recv_sem=recv_sems.at[k],
                device_id={"tp": peer},
                device_id_type=MESH,
            )
        )
    for copy in copies:
        copy.start()
    for copy in copies:
        copy.wait()
    total = mine[...]
    for k in range(n_tp - 1):
        total = total + theirs[k]
    scale = jnp.transpose(lax.rsqrt(total / (HEADS * DV) + EPS), (1, 0))
    for b in range(blocks):
        rows = slice(b * BLK, (b + 1) * BLK)
        out_ref[rows, :] = (combined[rows, :] * scale[:, b : b + 1] * gain_ref[...]).astype(BF16)


def cost(flops, moved):
    return pl.CostEstimate(flops=int(flops), bytes_accessed=int(moved), transcendentals=0)


def on_device(n_st, n_tp, tokens, w_query, w_key, w_value, w_decay, decay_rate, block_scale,
              w_rquery, w_gate, w_rkey, w_rvalue, query_gain, key_gain, out_gain, store,
              passage_ids):
    length, depth = tokens.shape
    num_blocks = length // BLK
    width = w_value.shape[1]
    heads = width // DV
    stores_here, passage_rows, _ = store.shape
    tile = 2 * BLK
    tall = 4 * BLK
    whole = lambda *shape: pl.BlockSpec(shape, lambda i, *_: (0,) * len(shape))
    any_spec = pl.BlockSpec(memory_space=pl.ANY)
    vmem = pl.BlockSpec(memory_space=pltpu.VMEM)

    def shift(values, by):
        return lax.ppermute(values, "st", [(s, (s + by) % n_st) for s in range(n_st)])

    read_query = pl.pallas_call(
        query_kernel,
        grid=(length // tall,),
        in_specs=[
            pl.BlockSpec((tall, depth), lambda i: (i, 0)),
            whole(depth, width),
            whole(1, DV),
        ],
        out_specs=pl.BlockSpec((tall, width), lambda i: (i, 0)),
        out_shape=jax.ShapeDtypeStruct((length, width), BF16),
        cost_estimate=cost(2 * length * depth * width, 6e6),
        name="query",
    )(tokens, w_rquery, query_gain.reshape(1, DV)).reshape(num_blocks, BLK, width)

    groups = range(1, n_st // PAIR)
    queries = [read_query] + [shift(read_query, PAIR * k) for k in groups]
    ids = [passage_ids] + [shift(passage_ids, PAIR * k) for k in groups]

    held_store, _ = lax.optimization_barrier((store, read_query))
    rows = stores_here * passage_rows
    made = pl.pallas_call(
        passage_kernel,
        grid=(rows // tall,),
        in_specs=[
            pl.BlockSpec((tall, depth), lambda i: (i, 0)),
            whole(depth, width),
            whole(depth, width),
            whole(1, DV),
        ],
        out_specs=pl.BlockSpec((tall, 2 * width), lambda i: (i, 0)),
        out_shape=jax.ShapeDtypeStruct((rows, 2 * width), BF16),
        cost_estimate=cost(4 * rows * depth * width, 1e7),
        name="passages",
    )(held_store.reshape(rows, depth), w_rkey, w_rvalue, key_gain.reshape(1, DV))
    made = made.reshape(stores_here, passage_rows, 2 * width)
    other = lax.ppermute(made, "st", [(s, s ^ 1) for s in range(n_st)])

    spare = -w_query.shape[1] % BLK
    if spare:
        w_query, w_key, w_decay = (
            jnp.pad(w, ((0, 0), (0, spare))) for w in (w_query, w_key, w_decay)
        )
        decay_rate = jnp.pad(decay_rate, (0, spare))
    dk = w_query.shape[1]
    half = length // 2

    def linear(first, values, state):
        return pl.pallas_call(
            functools.partial(gla_kernel, first // BLK),
            grid=(half // tile,),
            in_specs=[
                pl.BlockSpec(memory_space=pltpu.SMEM),
                pl.BlockSpec((tile, depth), lambda i: (i + first // tile, 0)),
                whole(1, dk),
                whole(width, dk),
            ]
            + [any_spec] * 5,
            out_specs=[pl.BlockSpec((tile, width), lambda i: (i, 0))] * 2 + [whole(width, dk)],
            out_shape=[jax.ShapeDtypeStruct((half, width), F32)] * 2
            + [jax.ShapeDtypeStruct((width, dk), F32)],
            scratch_shapes=[
                pltpu.VMEM((depth, 3 * dk + 2 * width), BF16),
                pltpu.VMEM((width, dk), F32),
                pltpu.SemaphoreType.DMA((5,)),
            ],
            cost_estimate=cost(4e9, 7e6),
            name="gla",
        )(block_scale, values, decay_rate.reshape(1, dk), state,
          w_query, w_key, w_decay, w_value, w_gate)

    early_tokens, _ = lax.optimization_barrier((tokens, made))
    gla_first, gate_first, state = linear(0, early_tokens, jnp.zeros((width, dk), F32))
    made, _ = lax.optimization_barrier((made, gla_first))

    request_count = passage_ids.shape[0] * passage_ids.shape[1]
    most = request_count // min(n_st, request_count // 2)

    def read(names, query):
        return pl.pallas_call(
            functools.partial(read_kernel, PAIR * most),
            in_specs=[
                pl.BlockSpec(memory_space=pltpu.SMEM), vmem, any_spec, any_spec,
            ],
            out_specs=[vmem, vmem],
            out_shape=[
                jax.ShapeDtypeStruct((num_blocks, BLK, width), BF16),
                jax.ShapeDtypeStruct((heads, num_blocks, BLK), F32),
            ],
            scratch_shapes=[
                pltpu.VMEM((2 * stores_here, passage_rows, 2 * width), BF16),
                pltpu.VMEM((num_blocks, BLK, width), F32),
                pltpu.VMEM((heads, num_blocks, 8, BLK), F32),
                pltpu.SMEM((request_count + 1,), jnp.int32),
                pltpu.SMEM((request_count + 1,), jnp.int32),
                pltpu.SemaphoreType.DMA((2,)),
            ],
            cost_estimate=cost(2e9, 5e6),
            name="reads",
        )(names, query, made, other)

    nums, dens = [], []
    for k in groups:
        num, den = read(ids[k], queries[k])
        tokens, _ = lax.optimization_barrier((tokens, num))
        nums.append(shift(num, -PAIR * k))
        dens.append(shift(den, -PAIR * k))

    gla_out, gate, _ = linear(half, tokens, state)
    read_query, gla_out = lax.optimization_barrier((read_query, gla_out))
    num, den = read(passage_ids, read_query)
    nums.append(num)
    dens.append(den)

    return pl.pallas_call(
        functools.partial(finish_kernel, len(nums), n_tp),
        in_specs=[vmem] + [any_spec] * (4 + len(nums)) + [vmem] * len(nums),
        out_specs=vmem,
        out_shape=jax.ShapeDtypeStruct((length, width), BF16),
        scratch_shapes=[pltpu.VMEM((length, width), F32)] * 2
        + [pltpu.VMEM((num_blocks, BLK, width), BF16)] * len(nums)
        + [
            pltpu.VMEM((length, width), F32),
            pltpu.VMEM((num_blocks, BLK), F32),
            pltpu.VMEM((max(n_tp - 1, 1), num_blocks, BLK), F32),
            pltpu.SemaphoreType.DMA((max(n_tp - 1, 1),)),
            pltpu.SemaphoreType.DMA((max(n_tp - 1, 1),)),
            pltpu.SemaphoreType.DMA((2 + len(nums), num_blocks)),
        ],
        compiler_params=pltpu.CompilerParams(collective_id=0, has_side_effects=True),
        cost_estimate=cost(1e9, 6e6),
        name="finish",
    )(out_gain.reshape(1, width), gla_first, gla_out, gate_first, gate, *nums, *dens)


def solution(mesh):
    def body(*args):
        return on_device(mesh.shape["st"], mesh.shape["tp"], *args)

    return jax.shard_map(
        body,
        mesh=mesh,
        in_specs=(
            P(("grp", "st"), None),
            P(None, "tp"),
            P(None, "tp"),
            P(None, "tp"),
            P(None, "tp"),
            P("tp"),
            P(("grp", "st")),
            P(None, "tp"),
            P(None, "tp"),
            P(None, "tp"),
            P(None, "tp"),
            P(),
            P(),
            P("tp"),
            P(("grp", "st"), None, None),
            P(("grp", "st"), None),
        ),
        out_specs=P(("grp", "st"), "tp"),
        check_vma=False,
    )
```

```python
import functools

import jax
import jax.numpy as jnp
from jax import lax
from jax.experimental import pallas as pl
from jax.experimental.pallas import tpu as pltpu
from jax.sharding import PartitionSpec as P


HEADS = 8
DK = 64
DV = 128
BLK = 128
PAIR = 2
EPS = 1e-06
F32 = jnp.float32
BF16 = jnp.bfloat16
MESH = pl.DeviceIdType.MESH
NT = (((1,), (1,)), ((), ()))
TN = (((0,), (0,)), ((), ()))


def head_norm(values, gain_row):
    return values * lax.rsqrt(jnp.mean(values * values, axis=-1, keepdims=True) + EPS) * gain_row


def split(values):
    high = values.astype(BF16)
    return high, (values - high.astype(F32)).astype(BF16)


def query_kernel(tok_ref, w_ref, gain_ref, out_ref):
    made = jnp.dot(tok_ref[...], w_ref[...], preferred_element_type=F32)
    for h in range(made.shape[1] // DV):
        cols = slice(h * DV, (h + 1) * DV)
        out_ref[:, cols] = head_norm(made[:, cols], gain_ref[...]).astype(BF16)


def passage_kernel(rows_ref, wk_ref, wv_ref, gain_ref, out_ref):
    rows = rows_ref[...]
    width = wk_ref.shape[1]
    keys = jnp.dot(rows, wk_ref[...], preferred_element_type=F32).astype(BF16).astype(F32)
    for h in range(width // DV):
        cols = slice(h * DV, (h + 1) * DV)
        out_ref[:, cols] = head_norm(keys[:, cols], gain_ref[...]).astype(BF16)
    out_ref[:, width:] = jnp.dot(rows, wv_ref[...], preferred_element_type=F32).astype(BF16)


def gla_kernel(
    first, scale_ref, tok_ref, rate_ref, wq, wk, wd, wv, wg, *refs
):
    *given, gla_ref, gate_ref, kept, w_all, state, sems = refs
    step = pl.program_id(0)
    dk = wq.shape[1]
    dv = wv.shape[1]

    copies = []
    at = 0
    for i, w in enumerate((wq, wk, wd, wv, wg)):
        copies.append(pltpu.make_async_copy(w, w_all.at[:, pl.ds(at, w.shape[1])], sems.at[i]))
        at += w.shape[1]

    @pl.when(step == 0)
    def _():
        for copy in copies:
            copy.start()
        state[...] = given[0][...] if given else jnp.zeros_like(state)
        for copy in copies[:3]:
            copy.wait()

    tok = tok_ref[...]
    small = jnp.dot(tok, w_all[:, : 3 * dk], preferred_element_type=F32)

    @pl.when(step == 0)
    def _():
        for copy in copies[3:]:
            copy.wait()

    large = jnp.dot(tok, w_all[:, 3 * dk :], preferred_element_type=F32)
    gate_ref[...] = jax.nn.sigmoid(large[:, dv:])
    row_id = lax.broadcasted_iota(jnp.int32, (BLK, BLK), 0)
    col_id = lax.broadcasted_iota(jnp.int32, (BLK, BLK), 1)
    causal = row_id >= col_id
    lower = causal.astype(F32)
    lower = jnp.concatenate([lower, lower], axis=1).astype(BF16)
    lane_head = lax.broadcasted_iota(jnp.int32, (BLK, dk), 1) // DK
    zero = jnp.zeros((), BF16)
    blocks = tok_ref.shape[0] // BLK
    spans = [slice(i * BLK, (i + 1) * BLK) for i in range(blocks)]
    heads = [slice(h * DV, (h + 1) * DV) for h in range(dv // DV)]
    cums = []
    for i, rows in enumerate(spans):
        pre = small[rows, 2 * dk : 3 * dk]
        block_scale = scale_ref[first + step * blocks + i]
        high, low = split(-2.0 * rate_ref[...] * jax.nn.sigmoid(pre) * block_scale)
        cums.append(
            jnp.dot(lower, jnp.concatenate([high, low], axis=0), preferred_element_type=F32)
        )
    queries, scores, ups, totals, values = [], [], [], [], []
    for rows, cum in zip(spans, cums):
        q, k = small[rows, :dk], small[rows, dk : 2 * dk]
        total = cum[BLK - 1 : BLK, :]
        totals.append(jnp.exp(total))
        q_high, q_low = split(q * (DK ** (-0.5)) * jnp.exp(cum))
        k_high, k_low = split(k * jnp.exp(-cum))
        k_twice = jnp.concatenate([k_high, k_high], axis=1)
        ups.append(split(k * jnp.exp(total - cum)))
        values.append(split(large[rows, :dv]))
        for h in range(len(heads)):
            own_high = jnp.where(lane_head == h, q_high, zero)
            own_low = jnp.where(lane_head == h, q_low, zero)
            q_h = jnp.concatenate([own_high, own_low], axis=1)
            queries.append(q_h)
            scores.append(
                lax.dot_general(q_h, k_twice, NT, preferred_element_type=F32)
                + lax.dot_general(own_high, k_low, NT, preferred_element_type=F32)
            )
    within, added = [], []
    for i in range(blocks):
        v_high, v_low = values[i]
        v_twice = jnp.concatenate([v_high, v_high], axis=0)
        for h, cols in enumerate(heads):
            high, low = split(jnp.where(causal, scores[i * len(heads) + h], 0.0))
            within.append(
                jnp.dot(
                    jnp.concatenate([high, low], axis=1),
                    v_twice[:, cols],
                    preferred_element_type=F32,
                )
                + jnp.dot(high, v_low[:, cols], preferred_element_type=F32)
            )
        up_high, up_low = ups[i]
        both = lax.dot_general(
            v_high, jnp.concatenate([up_high, up_low], axis=1), TN, preferred_element_type=F32
        )
        added.append(
            both[:, :dk]
            + both[:, dk:]
            + lax.dot_general(v_low, up_high, TN, preferred_element_type=F32)
        )
    held = state[...]
    for i, rows in enumerate(spans):
        held_high = held.astype(BF16)
        held_twice = jnp.concatenate([held_high, held_high], axis=1)
        for h, cols in enumerate(heads):
            n = i * len(heads) + h
            gla_ref[rows, cols] = within[n] + lax.dot_general(
                queries[n], held_twice[cols], NT, preferred_element_type=F32
            )
        held = held * totals[i] + added[i]
    state[...] = held
    kept[...] = held


def read_kernel(reads, ids_ref, q_ref, own_ref, other_ref, num_ref, den_ref,
                kv, num_acc, den_acc, list_b, list_r, sems):
    held = own_ref.shape[0]
    width = q_ref.shape[2]
    copies = [
        pltpu.make_async_copy(own_ref, kv.at[pl.ds(0, held)], sems.at[0]),
        pltpu.make_async_copy(other_ref, kv.at[pl.ds(held, held)], sems.at[1]),
    ]
    for copy in copies:
        copy.start()
    me = lax.axis_index("st")
    chip = lax.div(me, PAIR)
    num_acc[...] = jnp.zeros_like(num_acc)
    den_acc[...] = jnp.zeros_like(den_acc)
    count = jnp.int32(0)
    for b in range(ids_ref.shape[0]):
        for j in range(ids_ref.shape[1]):
            name = ids_ref[b, j]
            owner = lax.div(name, held)
            row = name - owner * held
            list_b[count] = jnp.int32(b)
            list_r[count] = jnp.where(owner == me, row, row + held)
            count = count + jnp.where(lax.div(owner, PAIR) == chip, 1, 0)
    for copy in copies:
        copy.wait()
    ones = jnp.ones((8, kv.shape[1]), BF16)
    group = 8 if reads % 8 == 0 else 4 if reads % 4 == 0 else 1
    heads = [(h, slice(h * DV, (h + 1) * DV)) for h in range(width // DV)]
    for first in range(0, reads, group):
        items = []
        for r in range(first, first + group):
            b, row = list_b[r], list_r[r]
            for h, cols in heads:
                score = lax.dot_general(
                    q_ref[b, :, cols], kv[row, :, cols], NT, preferred_element_type=F32
                )
                items.append((b, row, h, cols, score))
        exps = [jnp.exp(item[-1] * (DV ** (-0.5))).astype(BF16) for item in items]
        made = []
        for (b, row, h, cols, _), expd in zip(items, exps):
            value = kv[row, :, width + h * DV : width + (h + 1) * DV]
            made.append((
                jnp.dot(expd, value, preferred_element_type=F32),
                lax.dot_general(ones, expd, NT, preferred_element_type=F32),
            ))
        for (b, row, h, cols, _), (num, den) in zip(items, made):
            num_acc[b, :, cols] += num
            den_acc[h, b] += den
    num_ref[...] = num_acc[...].astype(BF16)
    for h in range(width // DV):
        for b in range(q_ref.shape[0]):
            den_ref[h, b : b + 1] = den_acc[h, b, 0:1]


def finish_kernel(parts, n_tp, *refs):
    gain_ref, gla_parts, gate_parts = refs[0], refs[1:3], refs[3:5]
    nums, dens = refs[5 : 5 + parts], refs[5 + parts : 5 + 2 * parts]
    out_ref, combined, mine, theirs, send_sems, recv_sems = refs[5 + 2 * parts :]
    blocks = mine.shape[0]
    half = blocks // 2
    me = lax.axis_index("tp")
    barrier = pltpu.get_barrier_semaphore()
    peers = [lax.rem(me + k, n_tp) for k in range(1, n_tp)]
    for peer in peers:
        pl.semaphore_signal(barrier, inc=1, device_id={"tp": peer}, device_id_type=MESH)
    heads = dens[0].shape[0]
    width = out_ref.shape[1]
    inverse = []
    for h in range(heads):
        den = dens[0][h]
        for extra in dens[1:]:
            den = den + extra[h]
        inverse.append(jnp.transpose(1.0 / den, (1, 0)))
    ones = jnp.ones((8, 2 * width), BF16)
    for b in range(blocks):
        rows = slice(b * BLK, (b + 1) * BLK)
        there = slice(b % half * BLK, (b % half + 1) * BLK)
        gla_ref, gate_ref = gla_parts[b // half], gate_parts[b // half]
        for h in range(heads):
            cols = slice(h * DV, (h + 1) * DV)
            num = nums[0][b, :, cols].astype(F32)
            for extra in nums[1:]:
                num = num + extra[b, :, cols].astype(F32)
            combined[rows, cols] = (
                gla_ref[there, cols] + gate_ref[there, cols] * (num * inverse[h][:, b : b + 1])
            )
        held = combined[rows, :]
        sums = lax.dot_general(
            ones, jnp.concatenate(split(held * held), axis=1), NT, preferred_element_type=F32
        )
        mine[b : b + 1, :] = sums[0:1]
    pl.semaphore_wait(barrier, n_tp - 1)
    copies = []
    for k, peer in enumerate(peers):
        copies.append(
            pltpu.make_async_remote_copy(
                src_ref=mine,
                dst_ref=theirs.at[k],
                send_sem=send_sems.at[k],
                recv_sem=recv_sems.at[k],
                device_id={"tp": peer},
                device_id_type=MESH,
            )
        )
    for copy in copies:
        copy.start()
    for copy in copies:
        copy.wait()
    total = mine[...]
    for k in range(n_tp - 1):
        total = total + theirs[k]
    scale = jnp.transpose(lax.rsqrt(total / (HEADS * DV) + EPS), (1, 0))
    for b in range(blocks):
        rows = slice(b * BLK, (b + 1) * BLK)
        out_ref[rows, :] = (combined[rows, :] * scale[:, b : b + 1] * gain_ref[...]).astype(BF16)


def cost(flops, moved):
    return pl.CostEstimate(flops=int(flops), bytes_accessed=int(moved), transcendentals=0)


def on_device(n_st, n_tp, tokens, w_query, w_key, w_value, w_decay, decay_rate, block_scale,
              w_rquery, w_gate, w_rkey, w_rvalue, query_gain, key_gain, out_gain, store,
              passage_ids):
    length, depth = tokens.shape
    num_blocks = length // BLK
    width = w_value.shape[1]
    heads = width // DV
    stores_here, passage_rows, _ = store.shape
    tile = 4 * BLK
    tall = 4 * BLK
    whole = lambda *shape: pl.BlockSpec(shape, lambda i, *_: (0,) * len(shape))
    any_spec = pl.BlockSpec(memory_space=pl.ANY)
    vmem = pl.BlockSpec(memory_space=pltpu.VMEM)

    def shift(values, by):
        return lax.ppermute(values, "st", [(s, (s + by) % n_st) for s in range(n_st)])

    read_query = pl.pallas_call(
        query_kernel,
        grid=(length // tall,),
        in_specs=[
            pl.BlockSpec((tall, depth), lambda i: (i, 0)),
            whole(depth, width),
            whole(1, DV),
        ],
        out_specs=pl.BlockSpec((tall, width), lambda i: (i, 0)),
        out_shape=jax.ShapeDtypeStruct((length, width), BF16),
        cost_estimate=cost(2 * length * depth * width, 6e6),
        name="query",
    )(tokens, w_rquery, query_gain.reshape(1, DV)).reshape(num_blocks, BLK, width)

    groups = range(1, n_st // PAIR)
    queries = [read_query] + [shift(read_query, PAIR * k) for k in groups]
    ids = [passage_ids] + [shift(passage_ids, PAIR * k) for k in groups]

    held_store, _ = lax.optimization_barrier((store, read_query))
    rows = stores_here * passage_rows
    made = pl.pallas_call(
        passage_kernel,
        grid=(rows // tall,),
        in_specs=[
            pl.BlockSpec((tall, depth), lambda i: (i, 0)),
            whole(depth, width),
            whole(depth, width),
            whole(1, DV),
        ],
        out_specs=pl.BlockSpec((tall, 2 * width), lambda i: (i, 0)),
        out_shape=jax.ShapeDtypeStruct((rows, 2 * width), BF16),
        cost_estimate=cost(4 * rows * depth * width, 1e7),
        name="passages",
    )(held_store.reshape(rows, depth), w_rkey, w_rvalue, key_gain.reshape(1, DV))
    made = made.reshape(stores_here, passage_rows, 2 * width)
    other = lax.ppermute(made, "st", [(s, s ^ 1) for s in range(n_st)])

    spare = -w_query.shape[1] % BLK
    if spare:
        w_query, w_key, w_decay = (
            jnp.pad(w, ((0, 0), (0, spare))) for w in (w_query, w_key, w_decay)
        )
        decay_rate = jnp.pad(decay_rate, (0, spare))
    dk = w_query.shape[1]
    half = length // 2

    def linear(first, values, *state):
        return pl.pallas_call(
            functools.partial(gla_kernel, first // BLK),
            grid=(half // tile,),
            in_specs=[
                pl.BlockSpec(memory_space=pltpu.SMEM),
                pl.BlockSpec((tile, depth), lambda i: (i + first // tile, 0)),
                whole(1, dk),
            ]
            + [any_spec] * 5
            + [whole(width, dk)] * len(state),
            out_specs=[pl.BlockSpec((tile, width), lambda i: (i, 0))] * 2 + [whole(width, dk)],
            out_shape=[jax.ShapeDtypeStruct((half, width), F32)] * 2
            + [jax.ShapeDtypeStruct((width, dk), F32)],
            scratch_shapes=[
                pltpu.VMEM((depth, 3 * dk + 2 * width), BF16),
                pltpu.VMEM((width, dk), F32),
                pltpu.SemaphoreType.DMA((5,)),
            ],
            cost_estimate=cost(4e9, 7e6),
            name="gla",
        )(block_scale, values, decay_rate.reshape(1, dk),
          w_query, w_key, w_decay, w_value, w_gate, *state)

    early_tokens, _ = lax.optimization_barrier((tokens, made))
    gla_first, gate_first, state = linear(0, early_tokens)
    made, _ = lax.optimization_barrier((made, gla_first))

    request_count = passage_ids.shape[0] * passage_ids.shape[1]
    most = request_count // min(n_st, request_count // 2)

    def read(names, query):
        return pl.pallas_call(
            functools.partial(read_kernel, PAIR * most),
            in_specs=[
                pl.BlockSpec(memory_space=pltpu.SMEM), vmem, any_spec, any_spec,
            ],
            out_specs=[vmem, vmem],
            out_shape=[
                jax.ShapeDtypeStruct((num_blocks, BLK, width), BF16),
                jax.ShapeDtypeStruct((heads, num_blocks, BLK), F32),
            ],
            scratch_shapes=[
                pltpu.VMEM((2 * stores_here, passage_rows, 2 * width), BF16),
                pltpu.VMEM((num_blocks, BLK, width), F32),
                pltpu.VMEM((heads, num_blocks, 8, BLK), F32),
                pltpu.SMEM((request_count + 1,), jnp.int32),
                pltpu.SMEM((request_count + 1,), jnp.int32),
                pltpu.SemaphoreType.DMA((2,)),
            ],
            cost_estimate=cost(2e9, 5e6),
            name="reads",
        )(names, query, made, other)

    nums, dens = [], []
    for k in groups:
        num, den = read(ids[k], queries[k])
        tokens, _ = lax.optimization_barrier((tokens, num))
        nums.append(shift(num, -PAIR * k))
        dens.append(shift(den, -PAIR * k))

    gla_out, gate, _ = linear(half, tokens, state)
    read_query, gla_out = lax.optimization_barrier((read_query, gla_out))
    num, den = read(passage_ids, read_query)
    nums.append(num)
    dens.append(den)

    return pl.pallas_call(
        functools.partial(finish_kernel, len(nums), n_tp),
        in_specs=[vmem] * (5 + 2 * len(nums)),
        out_specs=vmem,
        out_shape=jax.ShapeDtypeStruct((length, width), BF16),
        scratch_shapes=[
            pltpu.VMEM((length, width), F32),
            pltpu.VMEM((num_blocks, BLK), F32),
            pltpu.VMEM((max(n_tp - 1, 1), num_blocks, BLK), F32),
            pltpu.SemaphoreType.DMA((max(n_tp - 1, 1),)),
            pltpu.SemaphoreType.DMA((max(n_tp - 1, 1),)),
        ],
        compiler_params=pltpu.CompilerParams(collective_id=0, has_side_effects=True),
        cost_estimate=cost(1e9, 6e6),
        name="finish",
    )(out_gain.reshape(1, width), gla_first, gla_out, gate_first, gate, *nums, *dens)


def solution(mesh):
    def body(*args):
        return on_device(mesh.shape["st"], mesh.shape["tp"], *args)

    return jax.shard_map(
        body,
        mesh=mesh,
        in_specs=(
            P(("grp", "st"), None),
            P(None, "tp"),
            P(None, "tp"),
            P(None, "tp"),
            P(None, "tp"),
            P("tp"),
            P(("grp", "st")),
            P(None, "tp"),
            P(None, "tp"),
            P(None, "tp"),
            P(None, "tp"),
            P(),
            P(),
            P("tp"),
            P(("grp", "st"), None, None),
            P(("grp", "st"), None),
        ),
        out_specs=P(("grp", "st"), "tp"),
        check_vma=False,
    )
```
